32 devices in a mesh: sp: 8 (over z, y), tp: 4 (over x, core).
Axes of the slice: x: 2, y: 2, z: 4, core: 2. Of those that a mesh axis runs over, the one named last changes fastest.
Arguments:
- queries: bfloat16 [8192, 1024], P('sp', 'tp'), may hold values from -6 to 6
- keys: bfloat16 [8192, 1024], P('sp', 'tp'), may hold values from -6 to 6
- values: bfloat16 [8192, 1024], P('sp', 'tp'), may hold values from -6 to 6
- stick_bias: bfloat16 [8192, 8], P('sp', 'tp'), may hold values from -14 to 0
- residual: bfloat16 [8192, 2048], P(('sp', 'tp')), may hold values from -6 to 6
- out_weight: bfloat16 [1024, 2048], replicated, may hold values from -0.1875 to 0.1875
- norm_gain: float32 [2048], replicated, may hold values from 0.1 to 1.9
- gate_weight: bfloat16 [2048, 5632], P('sp', 'tp'), may hold values from -0.125 to 0.125
- value_weight: bfloat16 [2048, 5632], P('sp', 'tp'), may hold values from -0.125 to 0.125
- down_weight: bfloat16 [2048, 5632], P('sp', 'tp'), may hold values from -0.078125 to 0.078125
- conv_gate: float32 [3, 5632], P(None, 'tp'), may hold values from -3.5 to 3.5
- conv_value: float32 [3, 5632], P(None, 'tp'), may hold values from -3.5 to 3.5
Outputs:
- mixed: bfloat16 [8192, 2048], P(('sp', 'tp'))
The draws below stay inside these ranges and needn't reach their ends.
All inputs are finite; a program needn't handle non-finite values.
Results may differ from the reference program's by a relative error of at most 0.023.
Values may be sent and summed in bfloat16 or wider, within the bound.
A program may use at most 128 MiB of HBM per device.

```python
import jax
import jax.numpy as jnp
from jax import lax

D = 2048
FOCUS_CHANNELS = 8
HEAD_DIM = 128
FF = 5632
WIDTH = 3
TOK_DEV = 1024
STRING_LENGTH = 8192
N_TP = 4


def draw_values(key, part):
    mean_key, noise_key = jax.random.split(jax.random.fold_in(key, 7), 2)
    blocks = STRING_LENGTH // TOK_DEV
    means = 0.3 * jnp.clip(jax.random.normal(mean_key, (blocks, FOCUS_CHANNELS * HEAD_DIM), jnp.float32), -4.0, 4.0)
    noise = jnp.clip(jax.random.normal(noise_key, (STRING_LENGTH, FOCUS_CHANNELS * HEAD_DIM), jnp.float32), -4.0, 4.0)
    return (jnp.repeat(means, TOK_DEV, axis=0) + noise).astype(jnp.bfloat16)


def draw_stick_bias(key, part):
    complete_lookup_line = jax.random.split(jax.random.fold_in(key, 11), 5)
    blocks = STRING_LENGTH // TOK_DEV
    slow_share = 0.5
    lagging_fraction = jax.random.uniform(complete_lookup_line[0], (FOCUS_CHANNELS,), jnp.float32) < slow_share
    base = jnp.where(lagging_fraction, jnp.log(0.6 / STRING_LENGTH) - 2.5, jnp.log(1.0 / 40.0) - 2.5)
    block_shift = jax.random.uniform(complete_lookup_line[1], (blocks, FOCUS_CHANNELS), jnp.float32, -0.7, 0.7)
    jitter = jnp.clip(2.0 * jax.random.normal(complete_lookup_line[2], (STRING_LENGTH, FOCUS_CHANNELS), jnp.float32), -5.0, 5.0)
    spike_location = jax.random.randint(complete_lookup_line[3], (3,), 0, STRING_LENGTH)
    spike_displacement_jitter = jax.random.uniform(complete_lookup_line[4], (STRING_LENGTH, FOCUS_CHANNELS), jnp.float32, -0.7, 0.7)
    equality_indicator = jnp.any(jnp.arange(STRING_LENGTH)[:, None] == spike_location[None, :], axis=1)
    odds_correction = jnp.clip(base[None, :] + jnp.repeat(block_shift, TOK_DEV, axis=0) + jitter, -14.0, 0.0)
    odds_correction = jnp.where(equality_indicator[:, None] & lagging_fraction[None, :], -1.0 + 0.4 * spike_displacement_jitter, odds_correction)
    return odds_correction.astype(jnp.bfloat16)


def steps_of(stream_key, dims, shards, low, top_value):
    def one(position, blocks):
        draws = jax.random.uniform(jax.random.fold_in(jax.random.fold_in(stream_key, 6), position), (blocks,), jnp.float32, low / len(shards), top_value / len(shards))
        return jnp.repeat(jnp.exp(draws), dims[position] // blocks).reshape((-1,) + (1,) * (len(dims) - position - 1))

    level = one(*shards[0])
    for cut in shards[1:]:
        level = level * one(*cut)
    return level


def normal_values(rng, shape, deviation, limit, cuts=(), kind=jnp.bfloat16):
    drawn = jax.random.normal(rng, shape, jnp.float32) * deviation
    if len(cuts) > 0:
        drawn = steps_of(rng, shape, cuts, -0.22, 0.18) * drawn
    return jnp.clip(drawn, min=-limit, max=limit).astype(kind)


def setup_inputs(seed: int = 0) -> dict:
    key_of = jax.random.split(jax.random.key(seed), 13)
    return {
        "queries": normal_values(key_of[0], (STRING_LENGTH, FOCUS_CHANNELS * HEAD_DIM), 1.0, 6.0, ((0, 8), (1, 4))),
        "keys": normal_values(key_of[1], (STRING_LENGTH, FOCUS_CHANNELS * HEAD_DIM), 1.0, 6.0, ((0, 8), (1, 4))),
        "values": draw_values(jax.random.fold_in(key_of[12], 71), 0),
        "stick_bias": draw_stick_bias(jax.random.fold_in(key_of[12], 71), 0),
        "residual": normal_values(key_of[4], (STRING_LENGTH, D), 1.0, 6.0, ((0, 32),)),
        "out_weight": normal_values(key_of[5], (FOCUS_CHANNELS * HEAD_DIM, D), (FOCUS_CHANNELS * HEAD_DIM) ** -0.5, 0.1875),
        "norm_gain": jnp.clip(1.0 + 0.18 * jax.random.normal(key_of[6], (D,), jnp.float32), 0.1, 1.9),
        "gate_weight": normal_values(key_of[7], (D, FF), D ** -0.5, 0.125, ((0, 8), (1, 4))),
        "value_weight": normal_values(key_of[8], (D, FF), D ** -0.5, 0.125, ((0, 8), (1, 4))),
        "down_weight": normal_values(key_of[9], (D, FF), FF ** -0.5, 0.078125, ((0, 8), (1, 4))),
        "conv_gate": normal_values(key_of[10], (WIDTH, FF), WIDTH ** -0.5, 3.5, ((1, 4),), jnp.float32),
        "conv_value": normal_values(key_of[11], (WIDTH, FF), WIDTH ** -0.5, 3.5, ((1, 4),), jnp.float32),
    }


EPS = 1e-06

def round_keep(value):
    return lax.optimization_barrier(value.astype(jnp.bfloat16)).astype(jnp.float32)

def depthwise(upward, taps):
    extended = jnp.concatenate([jnp.zeros((2, upward.shape[1]), jnp.float32), upward.astype(jnp.float32)], axis=0)
    return taps[0] * extended[:-2] + taps[1] * extended[1:-1] + taps[2] * extended[2:]

def reference(queries, keys, values, stick_bias, residual, out_weight, norm_gain, gate_weight, value_weight, down_weight, conv_gate, conv_value):
    length = queries.shape[0]
    query_heads = queries.astype(jnp.float32).reshape(length, FOCUS_CHANNELS, HEAD_DIM).transpose(1, 0, 2)
    key_heads = keys.astype(jnp.float32).reshape(length, FOCUS_CHANNELS, HEAD_DIM).transpose(1, 0, 2)
    value_heads = values.astype(jnp.float32).reshape(length, FOCUS_CHANNELS, HEAD_DIM).transpose(1, 0, 2)
    bias_heads = stick_bias.astype(jnp.float32).T
    positions = jnp.arange(length, dtype=jnp.int32)
    blocks = length // TOK_DEV
    scale = HEAD_DIM ** (-0.5)

    def one_block(args):
        head, block = args
        query_block = lax.dynamic_slice_in_dim(query_heads[head], (block * TOK_DEV).astype(jnp.int32), TOK_DEV, 0)
        scores = jnp.dot(query_block, key_heads[head].T, preferred_element_type=jnp.float32) * scale + bias_heads[head][None, :]
        query_pos = block * TOK_DEV + jnp.arange(TOK_DEV, dtype=jnp.int32)
        before = positions[None, :] < query_pos[:, None]
        log_keep = jnp.where(before, jax.nn.log_sigmoid(-scores), 0.0)
        after = lax.cumsum(log_keep, axis=1, reverse=True) - log_keep
        stick = jnp.where(before, jnp.exp(jax.nn.log_sigmoid(scores) + after), 0.0)
        stick = round_keep(stick)
        return jnp.dot(stick, value_heads[head], preferred_element_type=jnp.float32)
    head_index = jnp.repeat(jnp.arange(FOCUS_CHANNELS, dtype=jnp.int32), blocks)
    block_index = jnp.tile(jnp.arange(blocks, dtype=jnp.int32), FOCUS_CHANNELS)
    outputs = lax.map(one_block, (head_index, block_index))
    attended = outputs.reshape(FOCUS_CHANNELS, length, HEAD_DIM).transpose(1, 0, 2).reshape(length, FOCUS_CHANNELS * HEAD_DIM).astype(jnp.bfloat16)
    group_cols = FOCUS_CHANNELS * HEAD_DIM // N_TP
    projected = jnp.zeros((length, D), jnp.float32)
    for group in range(N_TP):
        part = jnp.dot(attended[:, group * group_cols:(group + 1) * group_cols], out_weight[group * group_cols:(group + 1) * group_cols], preferred_element_type=jnp.float32)
        projected = projected + round_keep(part)
    middle = (residual.astype(jnp.float32) + projected).astype(jnp.bfloat16)
    middle_f = middle.astype(jnp.float32)
    normed = (middle_f * lax.rsqrt(lax.optimization_barrier(jnp.mean(middle_f * middle_f, axis=-1, keepdims=True)) + EPS) * norm_gain).astype(jnp.bfloat16)
    gate_up = jnp.dot(normed, gate_weight, preferred_element_type=jnp.float32).astype(jnp.bfloat16)
    value_up = jnp.dot(normed, value_weight, preferred_element_type=jnp.float32).astype(jnp.bfloat16)
    hidden = (jax.nn.silu(depthwise(gate_up, conv_gate)) * depthwise(value_up, conv_value)).astype(jnp.bfloat16)
    unit_cols = FF // N_TP
    down_total = jnp.zeros((length, D), jnp.float32)
    for group in range(N_TP):
        part = jnp.dot(hidden[:, group * unit_cols:(group + 1) * unit_cols], down_weight[:, group * unit_cols:(group + 1) * unit_cols].T, preferred_element_type=jnp.float32)
        down_total = down_total + round_keep(part)
    return (middle_f + down_total).astype(jnp.bfloat16)
```

```python
import functools
import math

import jax
import jax.numpy as jnp
import numpy as np
from jax import lax
from jax.experimental import pallas as pl
from jax.experimental.pallas import tpu as pltpu
from jax.sharding import PartitionSpec as P

EPS = 1e-06
LOG2E = math.log2(math.e)
LANES = 128
KEY_TILE = 256
QUERY_TILE = 512


def from_behind(block, axis, distance):
    devices = range(lax.axis_size(axis))
    route = [(i - distance, i) for i in devices if i - distance in devices]
    return lax.ppermute(block, axis, route)


def ring_walk(count):
    return [2 * i for i in range(count // 2)] + [2 * i + 1 for i in reversed(range(count // 2))]


def ring_owner(axis, distance):
    count = lax.axis_size(axis)
    index = lax.axis_index(axis)
    place = jnp.where(index % 2 == 0, index // 2, count - 1 - index // 2)
    place = (place - distance + count) % count
    return jnp.where(place < count // 2, 2 * place, 2 * (count - 1 - place) + 1)


class RingGather:
    def __init__(self, blocks, axis):
        self.axis, self.count, self.step = axis, lax.axis_size(axis), 0
        walk = ring_walk(self.count)
        self.forward = [(walk[i], walk[(i + 1) % self.count]) for i in range(self.count)]
        self.backward = [(b, a) for a, b in self.forward]
        self.steps = self.count // 2
        self.ahead, self.behind = list(blocks), list(blocks)
        self.got = [(list(blocks), 0)]

    def advance(self):
        if self.step == self.steps:
            return
        self.step += 1
        self.ahead = [lax.ppermute(b, self.axis, self.forward) for b in self.ahead]
        self.got.append((self.ahead, self.step))
        if self.step < self.count - self.step:
            self.behind = [lax.ppermute(b, self.axis, self.backward) for b in self.behind]
            self.got.append((self.behind, self.count - self.step))

    def tie(self, other):
        self.ahead, self.behind, other = lax.optimization_barrier((self.ahead, self.behind, other))
        return other

    def result(self):
        while self.step < self.steps:
            self.advance()
            self.ahead, self.behind = lax.optimization_barrier((self.ahead, self.behind))
        wholes = []
        for which, first in enumerate(self.got[0][0]):
            rows = first.shape[0]
            whole = jnp.zeros((self.count * rows,) + first.shape[1:], first.dtype)
            for blocks, distance in self.got:
                at = ring_owner(self.axis, distance) * rows
                whole = lax.dynamic_update_slice_in_dim(whole, blocks[which], at, 0)
            wholes.append(whole)
        return wholes


def to_chip(block, axis, distance):
    count = lax.axis_size(axis)
    return lax.ppermute(block, axis, [(i, (i + 2 * distance) % count) for i in range(count)])


def to_core(block, axis):
    return lax.ppermute(block, axis, [(i, i ^ 1) for i in range(lax.axis_size(axis))])


def both_cores(block, axis):
    core = lax.axis_index(axis) % 2
    other = to_core(block, axis)
    low = jnp.where(core == 0, block, other)
    high = jnp.where(core == 0, other, block)
    return jnp.concatenate([low, high], axis=0)


def project_up(normed, weights, axis):
    pairs = lax.axis_size(axis) // 2
    place = lax.axis_index(axis) // 2
    arrived = [normed] + [to_chip(normed, axis, k) for k in range(1, pairs)]
    rows = 2 * normed.shape[0]
    ups = [jnp.zeros((pairs * rows, w.shape[1]), jnp.bfloat16) for w in weights]
    for k, block in enumerate(arrived):
        chip = both_cores(block, axis)
        at = (place - k + pairs) % pairs * rows
        for which, w in enumerate(weights):
            up = jnp.dot(chip, w, preferred_element_type=jnp.float32).astype(jnp.bfloat16)
            ups[which] = lax.dynamic_update_slice_in_dim(ups[which], up, at, 0)
    return ups


def project_down(hidden, weight, axis):
    count = lax.axis_size(axis)
    pairs = count // 2
    place, core = lax.axis_index(axis) // 2, lax.axis_index(axis) % 2
    rows = hidden.shape[0] // count

    def chip_sum(target):
        mine = lax.dynamic_slice_in_dim(hidden, target * 2 * rows, 2 * rows, 0)
        terms = lax.dot_general(
            mine, weight, (((1,), (1,)), ((), ())), preferred_element_type=jnp.float32
        ).astype(jnp.bfloat16)
        keep = lax.dynamic_slice_in_dim(terms, core * rows, rows, 0)
        give = lax.dynamic_slice_in_dim(terms, (1 - core) * rows, rows, 0)
        return keep.astype(jnp.float32) + to_core(give, axis).astype(jnp.float32)

    parts = []
    for k in range(1, pairs):
        part = chip_sum((place + k) % pairs).astype(jnp.bfloat16)
        part, hidden = lax.optimization_barrier((part, hidden))
        parts.append(to_chip(part, axis, k))
    total = chip_sum(place)
    for part in parts:
        total = total + part.astype(jnp.float32)
    return total


def fit(size, most):
    return max(d for d in range(1, most + 1) if size % d == 0)


def interleave(rows, tile):
    count, width = rows.shape
    cut = rows.reshape(count // tile, 8, tile // 8, width)
    return cut.transpose(0, 2, 1, 3).reshape(count, width)


def pieces_of(value):
    left, out = value, []
    for _ in range(3):
        piece = float(np.asarray(left, dtype=jnp.bfloat16))
        out.append(piece)
        left -= piece
    return out


def attend_kernel(
    diagonal, heads, head_size, tile, *refs
):
    if diagonal:
        q_ref, k_ref, v_ref, b_ref, out_ref, log_ref, part_ref, stick_ref = refs
    else:
        q_ref, k_ref, v_ref, b_ref, in_ref, inlog_ref, done_ref, part_ref, stick_ref, out_ref, log_ref = refs
    queries_here = q_ref.shape[0]
    block_rows = v_ref.shape[1]
    per_block = block_rows // tile
    runs = tile // 8
    factor = head_size ** (-0.5) * LOG2E
    root = pieces_of(head_size**0.5)
    lane = lax.broadcasted_iota(jnp.int32, (queries_here, LANES), 1)
    ones = jnp.where(lane == 0, root[0], jnp.where(lane == 1, root[1], jnp.where(lane == 2, root[2], 0.0)))
    ones = ones.astype(jnp.bfloat16)
    sub = lax.broadcasted_iota(jnp.int32, (8, queries_here), 0)
    query_pos = pl.program_id(0) * queries_here + lax.broadcasted_iota(
        jnp.int32, (8, queries_here), 1
    )
    if diagonal:
        out_ref[...] = jnp.zeros_like(out_ref)
        log_ref[...] = jnp.zeros_like(log_ref)
    else:
        out_ref[...] = in_ref[...]
        log_ref[...] = inlog_ref[...]

    me = lax.axis_index("sp")

    def step(index, masked):
        block = index // per_block
        row = pl.multiple_of(index * tile, tile)
        start = index * tile
        column = pl.multiple_of((index % per_block) * tile, tile)
        for h in range(heads):
            hs = slice(h * head_size, (h + 1) * head_size)
            key = jnp.concatenate(
                [k_ref[pl.ds(row, tile), hs], jnp.broadcast_to(b_ref[pl.ds(row, tile), h : h + 1], (tile, LANES))], axis=1
            )
            query = jnp.concatenate([q_ref[:, hs], ones], axis=1)
            scores = lax.dot_general(
                key, query, (((1,), (1,)), ((), ())), preferred_element_type=jnp.float32
            )
            total = jnp.zeros((8, queries_here), jnp.float32)
            for j in reversed(range(runs)):
                z = scores[j * 8 : (j + 1) * 8, :] * factor
                drop = jnp.maximum(z, jnp.log2(1.0 + jnp.exp2(jnp.minimum(z, 120.0))))
                if masked:
                    before = start + sub * runs + j < query_pos
                    drop = jnp.where(before, drop, 0.0)
                total = total + drop
                part_ref[h, j * 8 : (j + 1) * 8, :] = z - total
            suffix = total
            every = total
            for d in (1, 2, 4):
                moved = pltpu.roll(suffix, 8 - d, 0)
                suffix = suffix + jnp.where(sub < 8 - d, moved, 0.0)
                every = every + pltpu.roll(every, d, 0)
            base = log_ref[h] + (suffix - total)
            log_ref[h] = log_ref[h] + every
            for j in range(0, runs, 2):
                pair = []
                for i in (j, j + 1):
                    stick = jnp.exp2(part_ref[h, i * 8 : (i + 1) * 8, :] - base)
                    if masked:
                        before = start + sub * runs + i < query_pos
                        stick = jnp.where(before, stick, 0.0)
                    pair.append(stick)
                stick_ref[h, j * 8 : (j + 2) * 8, :] = jnp.concatenate(pair, axis=0).astype(
                    jnp.bfloat16
                )
            value = v_ref[pl.ds(pl.multiple_of((block * heads + h) * head_size, head_size), head_size), pl.ds(column, tile)]
            out_ref[h] += jnp.dot(value, stick_ref[h], preferred_element_type=jnp.float32)

    if diagonal:
        below = pl.program_id(0) * (queries_here // tile)
        top = below + queries_here // tile

        def near(i, _):
            step(top - 1 - i, True)
            return 0

        lax.fori_loop(0, queries_here // tile, near, 0)
    else:
        below = me * per_block

    def far(i, _):
        step(below - 1 - i, False)
        return 0

    lax.fori_loop(0, below, far, 0)
    if not diagonal:
        for h in range(heads):
            done_ref[:, h * head_size : (h + 1) * head_size] = out_ref[h].T.astype(jnp.bfloat16)


def attend(queries, keys, values_t, bias, state, heads, tile, part=0):
    rows, width = queries.shape
    head_size = width // heads
    diagonal = state is None
    tq = fit(rows, QUERY_TILE)
    whole = pl.BlockSpec(memory_space=pltpu.VMEM)
    in_specs = [pl.BlockSpec((tq, width), lambda i: (i + part, 0)), whole, whole, whole]
    out_block = pl.BlockSpec((heads, head_size, tq), lambda i: (0, 0, i))
    log_block = pl.BlockSpec((heads, 8, tq), lambda i: (0, 0, i))
    scratch = [
        pltpu.VMEM((heads, tile, tq), jnp.float32),
        pltpu.VMEM((heads, tile, tq), jnp.bfloat16),
    ]
    visited = keys.shape[0] // (2 if diagonal else 1)
    cost = pl.CostEstimate(
        flops=4 * rows * visited * width * 3,
        bytes_accessed=4 * keys.size * 2,
        transcendentals=3 * rows * visited * heads,
    )
    if diagonal:
        out_shape = (
            jax.ShapeDtypeStruct((heads, head_size, rows), jnp.float32),
            jax.ShapeDtypeStruct((heads, 8, rows), jnp.float32),
        )
        out_specs = (out_block, log_block)
        args = (queries, keys, values_t, bias)
    else:
        in_specs += [
            pl.BlockSpec((heads, head_size, tq), lambda i: (0, 0, i + part)),
            pl.BlockSpec((heads, 8, tq), lambda i: (0, 0, i + part)),
        ]
        out_shape = jax.ShapeDtypeStruct((tq, width), jnp.bfloat16)
        out_specs = pl.BlockSpec((tq, width), lambda i: (i, 0))
        scratch += [
            pltpu.VMEM((heads, head_size, tq), jnp.float32),
            pltpu.VMEM((heads, 8, tq), jnp.float32),
        ]
        args = (queries, keys, values_t, bias) + tuple(state)
    return pl.pallas_call(
        functools.partial(attend_kernel, diagonal, heads, head_size, tile),
        grid=(rows // tq if diagonal else 1,),
        in_specs=in_specs,
        out_specs=out_specs,
        out_shape=out_shape,
        scratch_shapes=scratch,
        cost_estimate=cost,
        compiler_params=pltpu.CompilerParams(dimension_semantics=("arbitrary",), vmem_limit_bytes=60 * 2**20),
        name="attend_own" if diagonal else f"attend_past_{part}",
    )(*args)


def local(
    queries,
    keys,
    values,
    stick_bias,
    residual,
    out_weight,
    norm_gain,
    gate_weight,
    value_weight,
    down_weight,
    conv_gate,
    conv_value,
):
    rows_here = queries.shape[0]
    heads_here = stick_bias.shape[1]
    tile = fit(rows_here, KEY_TILE)
    key_own = interleave(keys, tile)
    value_own = interleave(values, tile).T
    bias_own = interleave(stick_bias, tile)
    key_all, value_all, bias_all = RingGather((key_own, value_own, bias_own), "sp").result()
    state = attend(queries, key_own, value_own, bias_own, None, heads_here, tile)
    late, key_all, value_all = lax.optimization_barrier(
        ((gate_weight, value_weight, down_weight), key_all, value_all)
    )
    gate_all = lax.all_gather(late[0], "sp", axis=0, tiled=True)
    ring = RingGather(late[1:], "sp")
    parts = rows_here // fit(rows_here, QUERY_TILE)
    attended = []
    for part in range(parts):
        ring.advance()
        done = attend(queries, key_all, value_all, bias_all, state, heads_here, tile, part)
        attended.append(done)
        if part + 1 < parts:
            done, state = ring.tie((done, state))
            attended[-1] = done
    attended = jnp.concatenate(attended, axis=0)
    row_heads = lax.all_to_all(attended, "tp", split_axis=0, concat_axis=1, tiled=True)
    projected = jnp.dot(row_heads, out_weight, preferred_element_type=jnp.float32)
    middle_f = (residual.astype(jnp.float32) + projected).astype(jnp.bfloat16).astype(jnp.float32)
    normed = (
        middle_f
        * lax.rsqrt(jnp.mean(middle_f * middle_f, axis=-1, keepdims=True) + EPS)
        * norm_gain
    ).astype(jnp.bfloat16)
    up_all, down_all = ring.result()
    gate_up, value_up = project_up(normed, (gate_all, up_all), "tp")
    rim_gate, rim_value = from_behind((gate_up[-2:], value_up[-2:]), "sp", 1)

    def depthwise(rim, upward, taps):
        extended = jnp.concatenate([rim, upward], axis=0).astype(jnp.float32)
        return taps[0] * extended[:-2] + taps[1] * extended[1:-1] + taps[2] * extended[2:]

    hidden = (
        jax.nn.silu(depthwise(rim_gate, gate_up, conv_gate))
        * depthwise(rim_value, value_up, conv_value)
    ).astype(jnp.bfloat16)
    down_total = project_down(hidden, down_all, "tp")
    return (middle_f + down_total).astype(jnp.bfloat16)


def solution(mesh):
    in_specs = (
        P("sp", "tp"),
        P("sp", "tp"),
        P("sp", "tp"),
        P("sp", "tp"),
        P(("sp", "tp"), None),
        P(),
        P(),
        P("sp", "tp"),
        P("sp", "tp"),
        P("sp", "tp"),
        P(None, "tp"),
        P(None, "tp"),
    )
    out_specs = P(("sp", "tp"), None)
    return jax.shard_map(local, mesh=mesh, in_specs=in_specs, out_specs=out_specs, check_vma=False)
```
